256 devices in a mesh: ep: 32 (over z, x), tp: 8 (over y, core).
Axes of the slice: x: 4, y: 4, z: 8, core: 2. Of those that a mesh axis runs over, the one named last changes fastest.
Arguments:
- tokens: bfloat16 [512, 2048], P('ep'), may hold values from -6 to 6
- lengths: int32 [512], P('ep'), may hold values from 1024 to 16384
- old_state: float32 [512, 8, 128, 128], P('ep', 'tp'), may hold values from -2 to 2
- query_weight: bfloat16 [2048, 1024], P(None, 'tp'), may hold values from -0.125 to 0.125
- key_weight: bfloat16 [2048, 1024], P(None, 'tp'), may hold values from -0.125 to 0.125
- value_weight: bfloat16 [2048, 1024], P(None, 'tp'), may hold values from -0.125 to 0.125
- gate_weight: bfloat16 [2048, 1024], P(None, 'tp'), may hold values from -0.125 to 0.125
- head_gain: float32 [1024], P('tp'), may hold values from 0.1 to 1.9
- output_weight: bfloat16 [1024, 2048], P('tp'), may hold values from -0.1875 to 0.1875
- first_gain: float32 [2048], replicated, may hold values from 0.1 to 1.9
- expert_ids: int32 [512, 6], P('ep'), may hold values from 0 to 63, all different within a row; in each aligned block of 16 rows (0 to 15, 16 to 31, ...) at most 2 rows name the same one
- expert_weights: float32 [512, 6], P('ep'), may hold values from 0.05 to 0.8
- expert_gate: bfloat16 [64, 2048, 512], P('ep', None, 'tp'), may hold values from -0.125 to 0.125
- expert_up: bfloat16 [64, 2048, 512], P('ep', None, 'tp'), may hold values from -0.125 to 0.125
- expert_down: bfloat16 [64, 512, 2048], P('ep', 'tp'), may hold values from -0.25 to 0.25
- shared_gate: bfloat16 [2048, 512], P(None, 'tp'), may hold values from -0.125 to 0.125
- shared_up: bfloat16 [2048, 512], P(None, 'tp'), may hold values from -0.125 to 0.125
- shared_down: bfloat16 [512, 2048], P('tp'), may hold values from -0.25 to 0.25
- side_gate: bfloat16 [2048], replicated, may hold values from -0.125 to 0.125
- dense_gate: bfloat16 [2048, 8192], P(None, ('ep', 'tp')), may hold values from -0.125 to 0.125
- dense_up: bfloat16 [2048, 8192], P(None, ('ep', 'tp')), may hold values from -0.125 to 0.125
- dense_down: bfloat16 [8192, 2048], P(('ep', 'tp')), may hold values from -0.25 to 0.25
- second_gain: float32 [2048], replicated, may hold values from 0.1 to 1.9
Outputs:
- layer_out: bfloat16 [512, 2048], P('ep')
- new_state: float32 [512, 8, 128, 128], P('ep', 'tp')
The draws below stay inside these ranges and needn't reach their ends.
Inputs may be any that keep to these rules, and one draw needn't show every extreme that they name: `expert_ids`: each row names 6 different experts. Among the 16 rows of one index of ep no expert is named by more than 2 rows, a bound that some block reaches.
All inputs are finite; a program needn't handle non-finite values.
Results may differ from the reference program's by a relative error of at most 0.017.
Values may be sent and summed in bfloat16 or wider, within the bound.
A program may use at most 64 MiB of HBM per device.

```python
import math
import jax
import jax.numpy as jnp
import numpy as np
from jax import lax

D = 2048
HEADS = 8
HD = 128
EFF = 512
SFF = 512
DENSE_FF = 8192
TOPK = 6
SEQ_DEV = 16
EXPERTS = 64
TOKENS = 512
CAP = 2
N_EP = 32
N_TP = 8


def set_ends(array, stream_key, low, high):
    extent = array.shape
    spot = [jax.random.randint(jax.random.fold_in(stream_key, axis), (), 0, extent[axis]) for axis in range(len(extent))]
    array = array.at[tuple(spot)].set(low)
    longest = extent.index(max(extent))
    spot[longest] = (spot[longest] + 1) % extent[longest]
    return array.at[tuple(spot)].set(high)


def levels(rng, extent, cuts, low, largest):
    gain, own = 1.0, jax.random.fold_in(rng, 6)
    for dim, parts in cuts:
        draws = jnp.exp(jax.random.uniform(jax.random.fold_in(own, dim), (parts,), jnp.float32, low / len(cuts), largest / len(cuts)))
        gain = gain * jnp.repeat(draws, extent[dim] // parts).reshape([-1 if axis == dim else 1 for axis in range(len(extent))])
    return gain


def deal_out(own_key, own, number, rows, amount, top, reach, lean):
    ranking = jax.random.permutation(own_key, amount)
    crowded, ordinary = shares(amount, rows * top, reach, lean, True), shares(amount, rows * top, reach, lean, False)
    places = jnp.arange(amount)

    def named(sizes, turn):
        used = int((sizes > 0).sum())
        fixed = max(1, used // 4)
        moved = fixed + (places - fixed + turn * (used - fixed)) % max(1, amount - fixed)
        return jnp.zeros((amount,), jnp.int32).at[ranking[jnp.where(places < fixed, places, moved)]].set(jnp.asarray(sizes, jnp.int32))

    sizes = jnp.where(number % 4 == 0, named(crowded, number // 4), named(ordinary, number - number // 4 - 1))
    mixed = jax.random.permutation(jax.random.fold_in(own, 3), amount)
    donor, receiver = mixed[0:amount // 2 * 2:2], mixed[1:amount // 2 * 2:2]
    margin = jnp.minimum(sizes[donor] - 1, reach - sizes[receiver]) // 2
    margin = jnp.where((donor == ranking[0]) | (receiver == ranking[0]) | (sizes[receiver] == 0), 0, jnp.maximum(margin, 0))
    moved = jax.random.randint(jax.random.fold_in(own, 4), (amount // 2,), 0, 1 << 20) % (margin + 1)
    sizes = sizes.at[donor].add(-moved).at[receiver].add(moved)
    items = jnp.searchsorted(jnp.cumsum(sizes), jnp.arange(rows * top), side="right").astype(jnp.int32)
    listing = items.reshape(top, rows).T
    listing = listing[jax.random.permutation(jax.random.fold_in(own, 1), rows)]
    turn = jax.random.randint(jax.random.fold_in(own, 2), (rows, 1), 0, top)
    return jnp.take_along_axis(listing, (jnp.arange(top)[None, :] + turn) % top, axis=1)


def shares(number_of, total, limit, lean, full):
    weights = [(1 << 20) // math.isqrt(standing ** lean) + 1 for standing in range(1, number_of + 1)]
    largest = limit if full else min(limit, max(-(-total // number_of), total * weights[0] // sum(weights)))
    least = 1 if total - largest >= number_of - 1 else 0
    counts, spare = [largest] + [least] * (number_of - 1), total - largest - least * (number_of - 1)
    while spare > 0:
        free = [i for i in range(1, number_of) if counts[i] < largest] or [i for i in range(1, number_of) if counts[i] < limit]
        pool, left = sum([weights[i] for i in free]), spare
        for i in free:
            extra = min(limit - counts[i], max(1, left * weights[i] // pool), spare)
            counts[i] = counts[i] + extra
            spare = spare - extra
    return np.array(counts)


def scatter_about(key, dims, width, limit, shards=(), held_as=jnp.bfloat16):
    factor_of = levels(key, dims, shards, -0.22, 0.18) if shards else 1.0
    drawn = jax.random.normal(key, dims, jnp.float32) * width * factor_of
    return jnp.minimum(jnp.maximum(drawn, -limit), limit).astype(held_as)


def setup_inputs(seed: int = 0) -> dict:
    key_of = jax.random.split(jax.random.key(seed), 24)
    tokens = scatter_about(key_of[0], (TOKENS, D), 1.0, 6.0, ((0, 32),))
    lengths = set_ends(jax.random.randint(key_of[1], (TOKENS,), 1024, 16385), jax.random.fold_in(key_of[1], 1), 1024, 16384).astype(jnp.int32)
    old_state = scatter_about(key_of[2], (TOKENS, HEADS, HD, HD), 0.25, 2.0, ((0, 32), (1, 8)), jnp.float32)
    query_weight = scatter_about(key_of[3], (D, HEADS * HD), D ** -0.5, 0.125, ((1, 8),))
    key_weight = scatter_about(key_of[4], (D, HEADS * HD), D ** -0.5, 0.125, ((1, 8),))
    value_weight = scatter_about(key_of[5], (D, HEADS * HD), D ** -0.5, 0.125, ((1, 8),))
    gate_weight = scatter_about(key_of[6], (D, HEADS * HD), D ** -0.5, 0.125, ((1, 8),))
    head_gain = jnp.clip(1.0 + 0.18 * jax.random.normal(key_of[7], (HEADS * HD,), jnp.float32), 0.1, 1.9)
    output_weight = scatter_about(key_of[8], (HEADS * HD, D), (HEADS * HD) ** -0.5, 0.1875, ((0, 8),))
    first_gain = jnp.clip(1.0 + 0.18 * jax.random.normal(key_of[9], (D,), jnp.float32), 0.1, 1.9)
    expert_ids_keys = jax.random.split(jax.random.fold_in(key_of[10], 1), TOKENS // SEQ_DEV)
    expert_ids_turns = jax.random.permutation(jax.random.fold_in(key_of[10], 3), TOKENS // SEQ_DEV)
    expert_ids = jax.vmap(lambda own, number: deal_out(jax.random.fold_in(key_of[10], 2), own, number, SEQ_DEV, EXPERTS, TOPK, CAP, 2))(expert_ids_keys, expert_ids_turns).reshape((TOKENS, TOPK))
    expert_weights = jnp.clip(jnp.exp(math.log(0.8) - 2.7725887 * jax.random.uniform(key_of[11], (TOKENS, TOPK), jnp.float32) ** levels(key_of[11], (TOKENS, TOPK), ((0, 32),), -0.2, 0.2)), 0.05, 0.8)
    expert_gate = scatter_about(key_of[12], (EXPERTS, D, EFF), D ** -0.5, 0.125, ((0, 32), (2, 8)))
    expert_up = scatter_about(key_of[13], (EXPERTS, D, EFF), D ** -0.5, 0.125, ((0, 32), (2, 8)))
    expert_down = scatter_about(key_of[14], (EXPERTS, EFF, D), EFF ** -0.5, 0.25, ((0, 32), (1, 8)))
    shared_gate = scatter_about(key_of[15], (D, SFF), D ** -0.5, 0.125, ((1, 8),))
    shared_up = scatter_about(key_of[16], (D, SFF), D ** -0.5, 0.125, ((1, 8),))
    shared_down = scatter_about(key_of[17], (SFF, D), SFF ** -0.5, 0.25, ((0, 8),))
    side_gate = scatter_about(key_of[18], (D,), D ** -0.5, 0.125)
    dense_gate = scatter_about(key_of[19], (D, DENSE_FF), D ** -0.5, 0.125, ((1, 256),))
    dense_up = scatter_about(key_of[20], (D, DENSE_FF), D ** -0.5, 0.125, ((1, 256),))
    dense_down = scatter_about(key_of[21], (DENSE_FF, D), (DENSE_FF // 16) ** -0.5, 0.25, ((0, 256),))
    second_gain = jnp.clip(1.0 + 0.18 * jax.random.normal(key_of[22], (D,), jnp.float32), 0.1, 1.9)
    return {"tokens": tokens, "lengths": lengths, "old_state": old_state, "query_weight": query_weight, "key_weight": key_weight, "value_weight": value_weight, "gate_weight": gate_weight, "head_gain": head_gain, "output_weight": output_weight, "first_gain": first_gain, "expert_ids": expert_ids, "expert_weights": expert_weights, "expert_gate": expert_gate, "expert_up": expert_up, "expert_down": expert_down, "shared_gate": shared_gate, "shared_up": shared_up, "shared_down": shared_down, "side_gate": side_gate, "dense_gate": dense_gate, "dense_up": dense_up, "dense_down": dense_down, "second_gain": second_gain}


NORM_EPS = 1e-05
RESIDUAL_SCALE = 2.0 ** 0.5

def rotate(inputs, positions):
    half_size = inputs.shape[-1] // 2
    frequency = 1.0 / 10000.0 ** (jnp.arange(half_size, dtype=jnp.float32) * 2.0 / inputs.shape[-1])
    angles = positions.astype(jnp.float32)[:, None] * frequency[None, :]
    cosine = jnp.cos(angles)[:, None, :]
    sine_part = jnp.sin(angles)[:, None, :]
    first_half = inputs[..., :half_size]
    second_half = inputs[..., half_size:]
    return jnp.concatenate([first_half * cosine - second_half * sine_part, first_half * sine_part + second_half * cosine], axis=-1)

def layer_norm(inputs, scale_gain):
    average = lax.optimization_barrier(jnp.mean(inputs, axis=-1, keepdims=True))
    centered = inputs - average
    variance = lax.optimization_barrier(jnp.mean(centered * centered, axis=-1, keepdims=True))
    return centered * lax.rsqrt(variance + NORM_EPS) * scale_gain

def reference(tokens, lengths, old_state, query_weight, key_weight, value_weight, gate_weight, head_gain, output_weight, first_gain, expert_ids, expert_weights, expert_gate, expert_up, expert_down, shared_gate, shared_up, shared_down, side_gate, dense_gate, dense_up, dense_down, second_gain):
    row_count = tokens.shape[0]
    head_count = old_state.shape[1]
    head_size = old_state.shape[-1]
    model_width = tokens.shape[1]
    queries = jnp.dot(tokens, query_weight, preferred_element_type=jnp.float32).reshape(row_count, head_count, head_size)
    keys_raw = jnp.dot(tokens, key_weight, preferred_element_type=jnp.float32).reshape(row_count, head_count, head_size)
    keys_raw = keys_raw * head_size ** (-0.5)
    values = jnp.dot(tokens, value_weight, preferred_element_type=jnp.float32).reshape(row_count, head_count, head_size)
    gating = jnp.dot(tokens, gate_weight, preferred_element_type=jnp.float32)
    query_rot = rotate(queries, lengths)
    key_rot = rotate(keys_raw, lengths)
    head_ids = jnp.arange(head_count, dtype=jnp.float32)
    decays = 1.0 - jnp.exp2(-2.0 - 10.0 * head_ids / (HEADS - 1))
    new_state = decays[None, :, None, None] * old_state + key_rot[:, :, :, None] * values[:, :, None, :]
    readout = jnp.einsum('thi,thij->thj', query_rot, new_state, precision=lax.Precision.HIGHEST)
    normed = layer_norm(readout, head_gain.reshape(head_count, head_size))
    mixed = (normed.reshape(row_count, head_count * head_size) * jax.nn.silu(gating)).astype(jnp.bfloat16)
    group_width = head_count * head_size // N_TP
    branch = jnp.zeros((row_count, model_width), jnp.float32)
    for shard_index in range(N_TP):
        lower = shard_index * group_width
        product = jnp.dot(mixed[:, lower:lower + group_width], output_weight[lower:lower + group_width], preferred_element_type=jnp.float32).astype(jnp.bfloat16)
        branch = branch + lax.optimization_barrier(product).astype(jnp.float32)
    after_mixer = layer_norm(RESIDUAL_SCALE * tokens.astype(jnp.float32) + branch, first_gain).astype(jnp.bfloat16)
    top_count = expert_ids.shape[1]
    expert_count = expert_gate.shape[0]
    slot_total = N_EP * CAP
    flat_ids = expert_ids.reshape(-1).astype(jnp.int32)
    pair_count = flat_ids.shape[0]
    onehot = (flat_ids[:, None] == jnp.arange(expert_count, dtype=jnp.int32)[None, :]).astype(jnp.int32)
    slot_rank = lax.optimization_barrier(jnp.sum(onehot * (jnp.cumsum(onehot, axis=0) - 1), axis=1))
    targets = (flat_ids * slot_total + slot_rank).astype(jnp.int32)
    owners = (jnp.arange(pair_count, dtype=jnp.int32) // top_count).astype(jnp.int32)
    table = jnp.zeros((expert_count * slot_total,), jnp.int32).at[targets].set(owners)
    gathered = after_mixer[table].reshape(expert_count, slot_total, model_width)
    hidden_width = expert_gate.shape[2] // N_TP

    def one_expert(operands):
        rows_in, gate_mat, up_mat, down_mat = operands
        gate_part = jnp.dot(rows_in, gate_mat, preferred_element_type=jnp.float32)
        up_part = jnp.dot(rows_in, up_mat, preferred_element_type=jnp.float32)
        hidden = (jax.nn.silu(gate_part) * up_part).astype(jnp.bfloat16)
        summed = jnp.zeros((rows_in.shape[0], model_width), jnp.float32)
        for shard_index in range(N_TP):
            lower = shard_index * hidden_width
            product = jnp.dot(hidden[:, lower:lower + hidden_width], down_mat[lower:lower + hidden_width], preferred_element_type=jnp.float32).astype(jnp.bfloat16)
            summed = summed + lax.optimization_barrier(product).astype(jnp.float32)
        return summed.astype(jnp.bfloat16)
    outputs = lax.map(one_expert, (gathered, expert_gate, expert_up, expert_down))
    picked = outputs.reshape(expert_count * slot_total, model_width)[targets].astype(jnp.float32)
    picked = picked.reshape(row_count, top_count, model_width)
    routed = lax.optimization_barrier(jnp.sum(picked * expert_weights[:, :, None], axis=1))
    switch = jax.nn.sigmoid(jnp.dot(after_mixer, side_gate, preferred_element_type=jnp.float32))
    dense_hidden = (jax.nn.silu(jnp.dot(after_mixer, dense_gate, preferred_element_type=jnp.float32)) * jnp.dot(after_mixer, dense_up, preferred_element_type=jnp.float32) * switch[:, None]).astype(jnp.bfloat16)
    shared_hidden = (jax.nn.silu(jnp.dot(after_mixer, shared_gate, preferred_element_type=jnp.float32)) * jnp.dot(after_mixer, shared_up, preferred_element_type=jnp.float32)).astype(jnp.bfloat16)
    side = (jnp.dot(dense_hidden, dense_down, preferred_element_type=jnp.float32) + jnp.dot(shared_hidden, shared_down, preferred_element_type=jnp.float32)).astype(jnp.bfloat16)
    total = RESIDUAL_SCALE * after_mixer.astype(jnp.float32) + routed + side.astype(jnp.float32)
    layer_out = layer_norm(total, second_gain).astype(jnp.bfloat16)
    return (layer_out, new_state)
```

```python
import functools

import jax
import jax.numpy as jnp
import numpy as np
from jax import lax
from jax.experimental import pallas as pl
from jax.experimental.pallas import tpu as pltpu
from jax.sharding import PartitionSpec as P

MESH = pl.DeviceIdType.MESH
NX, NY, NZ = 4, 4, 8
D = 2048
HD = 128
HEADS = 8
ROWS = 16
HALF = 8
QUARTER = D // NY
PART = QUARTER // 2
BLOCK = NZ * HALF
TOTAL = NX * BLOCK
NORM_EPS = 1e-05
SCALE = 2.0**0.5
BF16, F32 = jnp.bfloat16, jnp.float32
NT = (((1,), (1,)), ((), ()))
DECAYS = 1.0 - np.exp2(-2.0 - 10.0 * np.arange(HEADS) / (HEADS - 1))
FREQUENCY = (1.0 / 10000.0 ** (np.arange(HD // 2) * 2.0 / HD)).astype(np.float32)


def normed(rows, gain):
    centered = rows - jnp.mean(rows, axis=-1, keepdims=True)
    variance = jnp.mean(centered * centered, axis=-1, keepdims=True)
    return centered * lax.rsqrt(variance + NORM_EPS) * gain


def silu(v):
    return v * jax.nn.sigmoid(v)


def kernel(
    lens, tok_h, state_h, wq_h, wk_h, wv_h, wg_h, hgain_h, wo_h, g1_h, ids_h, ew_h, eg_h, eu_h, ed_h,
    sg_h, su_h, sd_h, side_h, dg_h, du_h, dd_h, g2_h, freq_h,
    out_ref, ns_h,
    tok, state, fresh, wm, hgain, wo, g1, g2, ids, ew, side, freq, wc, wd,
    ro, mx, rm, held, x_all, sc, wr, own, hid, pb, rya, rxb, s2a, s2b, r2a, r2b, z3, rz, gathered,
    in_sem, out_sem, send_sem, recv_sem,
):
    ep, tp = lax.axis_index("ep"), lax.axis_index("tp")
    z, x = ep // NX, ep % NX
    y, c = tp // 2, tp % 2
    here = x * NZ + z

    def at(ep_to, tp_to):
        return {"ep": ep_to, "tp": tp_to}

    def tp_peer(r):
        return at(ep, (tp + r) % 8)

    def y_peer(dy):
        return at(ep, (tp + 2 * dy) % 8)

    def x_peer(dx):
        return at(z * NX + (x + dx) % NX, tp)

    def z_peer(dz):
        return at(((z + dz) % NZ) * NX + x, tp)

    partner = at(ep, tp + 1 - 2 * c)
    barrier = pltpu.get_barrier_semaphore()
    peers = (
        [tp_peer(r) for r in range(1, 8)]
        + [x_peer(d) for d in range(1, NX)]
        + [z_peer(d) for d in range(1, NZ)]
    )
    for peer in peers:
        pl.semaphore_signal(barrier, inc=1, device_id=peer, device_id_type=MESH)

    numbers = {"in": 0, "remote": 0}
    sent = []

    def load(src, dst):
        copy = pltpu.make_async_copy(src, dst, in_sem.at[numbers["in"]])
        numbers["in"] += 1
        copy.start()
        return copy

    def send(src, dst, peer):
        n = numbers["remote"]
        numbers["remote"] += 1
        copy = pltpu.make_async_remote_copy(
            src_ref=src, dst_ref=dst, send_sem=send_sem.at[n], recv_sem=recv_sem.at[n], device_id=peer,
            device_id_type=MESH,
        )
        copy.start()
        sent.append(copy)
        return copy

    small = [load(ids_h, ids), load(ew_h, ew)]
    first = [load(tok_h, tok)]
    for k, w in enumerate((wq_h, wk_h, wv_h, wg_h)):
        first.append(load(w, wm.at[:, pl.ds(k * HD, HD)]))
    first.append(load(freq_h, freq))
    second = [load(state_h, state), load(hgain_h, hgain), load(wo_h, wo)]
    later = [load(g1_h, g1), load(g2_h, g2), load(side_h, side)]
    pl.semaphore_wait(barrier, len(peers))

    for copy in small:
        copy.wait()
    lane = lax.broadcasted_iota(jnp.int32, (HALF, HD), 1)
    rows_c = pl.ds(pl.multiple_of(c * HALF, HALF), HALF)
    my_ids, my_ew = ids[rows_c, :], ew[rows_c, :]
    table = jnp.zeros((HALF, HD), F32)
    for k in range(6):
        table += jnp.where(lane == my_ids[:, k : k + 1], my_ew[:, k : k + 1], 0.0)
    wr[here] = table
    table_z = [send(wr.at[here], wr.at[here], z_peer(d)) for d in range(1, NZ)]

    arrivals = []
    for src, dst, row, size in (
        (eg_h.at[0], wc, 0, 64), (eg_h.at[1], wc, 128, 64), (eu_h.at[0], wc, 256, 64), (eu_h.at[1], wc, 384, 64),
        (sg_h, wc, 512, 64), (su_h, wc, 640, 64), (dg_h, wc, 768, 32), (du_h, wc, 832, 32),
        (ed_h.at[0], wd, 0, 64), (ed_h.at[1], wd, 128, 64), (sd_h, wd, 256, 64), (dd_h, wd, 384, 32),
    ):
        later.append(load(src, dst.at[pl.ds(row, size), :]))
        arrivals.append(send(src, dst.at[pl.ds(row + size, size), :], partner))
    wd[448:512, :] = jnp.zeros((64, D), BF16)

    for copy in first:
        copy.wait()
    tokens = tok[...].astype(F32).reshape(ROWS, D).astype(BF16)
    projected = jnp.dot(tokens, wm[...], preferred_element_type=F32)
    queries, keys = projected[:, :HD], projected[:, HD : 2 * HD] * HD ** (-0.5)
    values, gating = projected[:, 2 * HD : 3 * HD], projected[:, 3 * HD :]
    row_of = lax.broadcasted_iota(jnp.int32, (ROWS, HD), 0)
    lane_of = lax.broadcasted_iota(jnp.int32, (ROWS, HD), 1)
    position = jnp.zeros((ROWS, HD), jnp.int32)
    for t in range(ROWS):
        position = jnp.where(row_of == t, lens[t], position)
    angles = position.astype(F32) * freq[...]
    cosine = jnp.cos(angles)
    sine = jnp.where(lane_of < HD // 2, -1.0, 1.0) * jnp.sin(angles)
    query_rot = queries * cosine + pltpu.roll(queries, HD // 2, 1) * sine
    key_rot = keys * cosine + pltpu.roll(keys, HD // 2, 1) * sine
    decay = jnp.float32(0.0)
    for h in range(HEADS):
        decay = decay + jnp.where(tp == h, jnp.float32(DECAYS[h]), jnp.float32(0.0))
    q_columns, k_columns = query_rot.T, key_rot.T
    for copy in second:
        copy.wait()
    for t in range(ROWS):
        new = decay * state[t] + k_columns[:, t : t + 1] * values[t : t + 1, :]
        fresh[t] = new
        ro[t : t + 1, :] = jnp.sum(q_columns[:, t : t + 1] * new, axis=0, keepdims=True)
    state_out = pltpu.make_async_copy(fresh, ns_h, out_sem.at[0])
    state_out.start()
    mixed = (normed(ro[...], hgain[...]) * silu(gating)).astype(BF16)
    share = jnp.dot(mixed, wo[...], preferred_element_type=F32)
    mx[...] = share.reshape(2, HALF, D).astype(BF16)

    cols = pl.ds(pl.multiple_of(y * QUARTER, QUARTER), QUARTER)
    shares = []
    for r in range(1, 8):
        to = (tp + r) % 8
        cols_to = pl.ds(pl.multiple_of((to // 2) * QUARTER, QUARTER), QUARTER)
        shares.append(send(mx.at[to % 2, :, cols_to], rm.at[r - 1], tp_peer(r)))
    for copy in table_z:
        copy.wait_recv()
    group = pl.ds(pl.multiple_of(x * NZ, NZ), NZ)
    table_x = [send(wr.at[group], wr.at[group], x_peer(d)) for d in range(1, NX)]
    total = SCALE * tok[c, :, cols].astype(F32) + mx[c, :, cols].astype(F32)
    for r in range(1, 8):
        shares[r - 1].wait_recv()
        total += rm[r - 1].astype(F32)
    held[here, :, cols] = total.astype(BF16)

    gather_z = [send(held.at[here, :, cols], held.at[here, :, cols], z_peer(d)) for d in range(1, NZ)]
    for copy in gather_z:
        copy.wait_recv()
    piece = held.at[group, :, cols]
    by_x, by_y = {}, {}
    for d in (2, 1, 3):
        by_x[d] = send(piece, piece, x_peer(d))
        by_y[d] = send(piece, piece, y_peer(d))
    second_level = []
    for d in (1, 3, 2):
        by_x[d].wait_recv()
        group_d = pl.ds(pl.multiple_of(((x + NX - d) % NX) * NZ, NZ), NZ)
        cols_a = pl.ds(pl.multiple_of(y * QUARTER, PART), PART)
        piece = held.at[group_d, :, cols_a]
        for e in (2, 1, 3):
            second_level.append(send(piece, piece, y_peer(e)))
        by_y[d].wait_recv()
        cols_b = pl.ds(pl.multiple_of(((y + NY - d) % NY) * QUARTER + PART, PART), PART)
        piece = held.at[group, :, cols_b]
        for e in (2, 1, 3):
            second_level.append(send(piece, piece, x_peer(e)))
    for copy in table_x:
        copy.wait_recv()
    for copy in later:
        copy.wait()
    for copy in arrivals:
        copy.wait_recv()
    for copy in second_level:
        copy.wait_recv()

    lanes = lax.broadcasted_iota(jnp.int32, (ROWS, HD), 1)

    def norm_step(i, carry):
        rows = held[pl.ds(2 * i, 2)].astype(F32).reshape(ROWS, D)
        after = normed(rows, g1[...]).astype(BF16)
        x_all[pl.ds(pl.multiple_of(i * ROWS, ROWS), ROWS), :] = after
        switch = jax.nn.sigmoid(jnp.sum(after.astype(F32) * side[...], axis=-1, keepdims=True))
        tables = wr[pl.ds(2 * i, 2)].reshape(ROWS, HD)
        w0 = jnp.sum(jnp.where(lanes == 2 * ep, tables, 0.0), axis=-1, keepdims=True)
        w1 = jnp.sum(jnp.where(lanes == 2 * ep + 1, tables, 0.0), axis=-1, keepdims=True)
        sc[pl.ds(pl.multiple_of(i * ROWS, ROWS), ROWS), :] = jnp.where(
            lanes == 0, w0, jnp.where(lanes == 1, w1, switch)
        )
        return carry

    lax.fori_loop(0, TOTAL // ROWS, norm_step, 0)
    own[...] = normed(held[here].astype(F32), g1[...])

    gates = lax.dot_general(x_all[...], wc[0:256, :], NT, preferred_element_type=F32)
    ups = lax.dot_general(x_all[...], wc[256:512, :], NT, preferred_element_type=F32)
    for e in range(2):
        lo, hi = e * HD, (e + 1) * HD
        hid[:, lo:hi] = (silu(gates[:, lo:hi]) * ups[:, lo:hi] * sc[:, e : e + 1]).astype(BF16)
    both = lax.dot_general(x_all[...], wc[512:768, :], NT, preferred_element_type=F32)
    block_of = lax.broadcasted_iota(jnp.int32, (TOTAL, HD), 0) // HALF
    shared = jnp.where(block_of == here, silu(both[:, :HD]) * both[:, HD:], 0.0)
    hid[:, 256:384] = shared.astype(BF16)
    wide = lax.dot_general(x_all[...], wc[768:896, :], NT, preferred_element_type=F32)
    wide_lane = lax.broadcasted_iota(jnp.int32, (TOTAL, HD), 1)
    dense = silu(wide) * pltpu.roll(wide, HD // 2, 1) * sc[:, 2:3]
    hid[:, 384:512] = jnp.where(wide_lane < HD // 2, dense, 0.0).astype(BF16)

    def rows_of(dx):
        return pl.ds(pl.multiple_of(((x + dx) % NX) * BLOCK, BLOCK), BLOCK)

    first_a, first_b = {}, {}
    for dy in (2, 1, 3, 0):
        base = ((y + dy) % NY) * QUARTER
        pair = pl.ds(pl.multiple_of(base, QUARTER), QUARTER)
        product = jnp.dot(hid[...], wd[:, pair], preferred_element_type=F32)
        pb[:, pair] = product.astype(BF16)
        for dx in (2, 1, 3, 0):
            if dy:
                piece = pb.at[rows_of(dx), pl.ds(pl.multiple_of(base, PART), PART)]
                first_a[dx, dy] = send(piece, rya.at[dy - 1, dx], y_peer(dy))
            if dx:
                piece = pb.at[rows_of(dx), pl.ds(pl.multiple_of(base + PART, PART), PART)]
                first_b[dx, dy] = send(piece, rxb.at[dx - 1, dy], x_peer(dx))
    second_a, second_b = {}, {}
    for d in (2, 1, 3, 0):
        part_a = pb[rows_of(d), pl.ds(pl.multiple_of(y * QUARTER, PART), PART)].astype(F32)
        for e in (1, 3, 2):
            first_a[d, e].wait_recv()
            part_a += rya[e - 1, d].astype(F32)
        if d:
            s2a[d - 1] = part_a.astype(BF16)
            second_a[d] = send(s2a.at[d - 1], r2a.at[d - 1], x_peer(d))
        cols_b = pl.ds(pl.multiple_of(((y + d) % NY) * QUARTER + PART, PART), PART)
        part_b = pb[rows_of(0), cols_b].astype(F32)
        for e in (1, 3, 2):
            first_b[e, d].wait_recv()
            part_b += rxb[e - 1, d].astype(F32)
        if d:
            s2b[d - 1] = part_b.astype(BF16)
            second_b[d] = send(s2b.at[d - 1], r2b.at[d - 1], y_peer(d))
    for d in (1, 3, 2):
        second_a[d].wait_recv()
        part_a += r2a[d - 1].astype(F32)
        second_b[d].wait_recv()
        part_b += r2b[d - 1].astype(F32)
    z3[:, :, :PART] = part_a.reshape(NZ, HALF, PART).astype(BF16)
    z3[:, :, PART:] = part_b.reshape(NZ, HALF, PART).astype(BF16)
    last = [send(z3.at[(z + d) % NZ], rz.at[d - 1], z_peer(d)) for d in range(1, NZ)]
    total = SCALE * own[:, cols].astype(BF16).astype(F32) + z3[z].astype(F32)
    for d in range(1, NZ):
        last[d - 1].wait_recv()
        total += rz[d - 1].astype(F32)
    gathered[c, :, cols] = total.astype(BF16)
    finals = [send(gathered.at[c, :, cols], gathered.at[c, :, cols], tp_peer(r)) for r in range(1, 8)]
    for copy in finals:
        copy.wait_recv()
    out_ref[...] = normed(gathered[...].astype(F32).reshape(ROWS, D), g2[...]).astype(BF16)
    for copy in sent:
        copy.wait_send()
    state_out.wait()


def per_device(
    tokens, lengths, old_state, query_weight, key_weight, value_weight, gate_weight, head_gain, output_weight,
    first_gain, expert_ids, expert_weights, expert_gate, expert_up, expert_down, shared_gate, shared_up,
    shared_down, side_gate, dense_gate, dense_up, dense_down, second_gain,
):
    frequency = jnp.asarray(np.concatenate([FREQUENCY, FREQUENCY])[None, :])
    anywhere = pl.BlockSpec(memory_space=pl.ANY)
    vmem = pltpu.VMEM
    out, fresh = pl.pallas_call(
        kernel,
        out_shape=(
            jax.ShapeDtypeStruct((ROWS, D), BF16),
            jax.ShapeDtypeStruct((ROWS, HD, HD), F32),
        ),
        in_specs=[pl.BlockSpec(memory_space=pltpu.SMEM)] + [anywhere] * 23,
        out_specs=(pl.BlockSpec(memory_space=pltpu.VMEM), anywhere),
        scratch_shapes=[
            vmem((2, HALF, D), BF16),
            vmem((ROWS, HD, HD), F32),
            vmem((ROWS, HD, HD), F32),
            vmem((D, 4 * HD), BF16),
            vmem((1, HD), F32),
            vmem((HD, D), BF16),
            vmem((1, D), F32),
            vmem((1, D), F32),
            vmem((ROWS, 6), jnp.int32),
            vmem((ROWS, 6), F32),
            vmem((1, D), F32),
            vmem((1, HD), F32),
            vmem((896, D), BF16),
            vmem((512, D), BF16),
            vmem((ROWS, HD), F32),
            vmem((2, HALF, D), BF16),
            vmem((7, HALF, QUARTER), BF16),
            vmem((NX * NZ, HALF, D), BF16),
            vmem((TOTAL, D), BF16),
            vmem((TOTAL, HD), F32),
            vmem((NX * NZ, HALF, HD), F32),
            vmem((HALF, D), F32),
            vmem((TOTAL, 512), BF16),
            vmem((TOTAL, D), BF16),
            vmem((3, 4, BLOCK, PART), BF16),
            vmem((3, 4, BLOCK, PART), BF16),
            vmem((3, BLOCK, PART), BF16),
            vmem((3, BLOCK, PART), BF16),
            vmem((3, BLOCK, PART), BF16),
            vmem((3, BLOCK, PART), BF16),
            vmem((NZ, HALF, QUARTER), BF16),
            vmem((7, HALF, QUARTER), BF16),
            vmem((2, HALF, D), BF16),
            pltpu.SemaphoreType.DMA((26,)),
            pltpu.SemaphoreType.DMA((1,)),
            pltpu.SemaphoreType.DMA((106,)),
            pltpu.SemaphoreType.DMA((106,)),
        ],
        compiler_params=pltpu.CompilerParams(
            collective_id=0, has_side_effects=True, vmem_limit_bytes=60 * 1024 * 1024
        ),
    )(
        lengths,
        tokens.reshape(2, HALF, D),
        old_state.reshape(ROWS, HD, HD),
        query_weight,
        key_weight,
        value_weight,
        gate_weight,
        head_gain.reshape(1, HD),
        output_weight,
        first_gain.reshape(1, D),
        expert_ids,
        expert_weights,
        expert_gate.transpose(0, 2, 1),
        expert_up.transpose(0, 2, 1),
        expert_down,
        shared_gate.T,
        shared_up.T,
        shared_down,
        side_gate.astype(F32).reshape(1, D),
        dense_gate.T,
        dense_up.T,
        dense_down,
        second_gain.reshape(1, D),
        frequency,
    )
    return out, fresh.reshape(ROWS, 1, HD, HD)


def solution(mesh):
    return jax.shard_map(
        per_device,
        mesh=mesh,
        in_specs=(
            P("ep", None), P("ep"), P("ep", "tp", None, None),
            P(None, "tp"), P(None, "tp"), P(None, "tp"), P(None, "tp"),
            P("tp"), P("tp", None), P(), P("ep", None), P("ep", None),
            P("ep", None, "tp"), P("ep", None, "tp"), P("ep", "tp", None),
            P(None, "tp"), P(None, "tp"), P("tp", None), P(),
            P(None, ("ep", "tp")), P(None, ("ep", "tp")), P(("ep", "tp"), None), P(),
        ),
        out_specs=(P("ep", None), P("ep", "tp", None, None)),
        check_vma=False,
    )
```
